32 devices in a mesh: fs: 4 (over y, x), tp: 8 (over z, core).
Axes of the slice: x: 2, y: 2, z: 4, core: 2. Of those that a mesh axis runs over, the one named last changes fastest.
Arguments:
- tokens: bfloat16 [4096, 2048], P(('fs', 'tp')), may hold values from -6 to 6
- up_gate: bfloat16 [4096, 5632], P('fs', 'tp'), may hold values from -8 to 8
- up_val: bfloat16 [4096, 5632], P('fs', 'tp'), may hold values from -6 to 6
- gate_weight: bfloat16 [2048, 5632], P('fs', 'tp'), may hold values from -0.125 to 0.125
- val_weight: bfloat16 [2048, 5632], P('fs', 'tp'), may hold values from -0.125 to 0.125
- gate_taps: bfloat16 [3, 5632], P(None, 'tp'), may hold values from -3 to 3
- val_taps: bfloat16 [3, 5632], P(None, 'tp'), may hold values from -3 to 3
- hidden_grad: bfloat16 [4096, 5632], P('fs', 'tp'), may hold values from -6 to 6
Outputs:
- input_grad: bfloat16 [4096, 2048], P(('fs', 'tp'))
- gate_weight_grad: float32 [2048, 5632], P('fs', 'tp')
- val_weight_grad: float32 [2048, 5632], P('fs', 'tp')
- gate_taps_grad: float32 [3, 5632], P(None, 'tp')
- val_taps_grad: float32 [3, 5632], P(None, 'tp')
- gate_row_norms: float32 [2048], P('fs')
- val_row_norms: float32 [2048], P('fs')
- tap_row_norms: float32 [2, 3], replicated
The draws below stay inside these ranges and needn't reach their ends.
All inputs are finite; a program needn't handle non-finite values.
Results may differ from the reference program's by a relative error of at most 0.017.
Values may be sent and summed in bfloat16 or wider, within the bound.
No kernel may reach another device: no remote copies, remote signals or barrier semaphores. Data moves between devices by JAX's collectives and lax.ppermute only.
A program may use at most 128 MiB of HBM per device.

```python
import jax
import jax.numpy as jnp
from jax import lax

D = 2048
FF = 5632
TAPS = 3
SEQ = 1024
TOKENS = 4096
N_TP = 8


def spiked(entries, stream_key, source, target, parts, factor):
    owner, partner = [(jnp.arange(entries.shape[axis_at]) // (entries.shape[axis_at] // parts)).reshape([-1 if axis == axis_at else 1 for axis in range(entries.ndim)]) for axis_at in (source, target)]
    chosen = jax.random.permutation(stream_key, parts)[partner]
    strong = (owner == chosen) | (owner == (partner + parts // 2) % parts)
    return jnp.where(strong, factor * entries, entries)


def shard_levels(stream_key, dims, shards, smallest, top_value):
    def one(dim, parts):
        steps = jax.random.uniform(jax.random.fold_in(jax.random.fold_in(stream_key, 6), dim), (parts,), jnp.float32, smallest / len(shards), top_value / len(shards))
        return jnp.repeat(jnp.exp(steps), dims[dim] // parts).reshape((-1,) + (1,) * (len(dims) - dim - 1))

    factor_of = one(*shards[0])
    for cut in shards[1:]:
        factor_of = factor_of * one(*cut)
    return factor_of


def scatter_about(rng, shape, width, most, split=(), kind=jnp.bfloat16):
    entries = jax.random.normal(rng, shape, jnp.float32) * width
    if len(split) > 0:
        entries = shard_levels(rng, shape, split, -0.22, 0.18) * entries
    return jnp.clip(entries, min=-most, max=most).astype(kind)


def noise_with(own_key, shape, spread, most, pieces, heavy, kind=jnp.bfloat16):
    drawn = spread * jax.random.normal(own_key, shape, jnp.float32)
    if pieces:
        drawn = drawn * shard_levels(own_key, shape, pieces, -0.22, 0.18)
    return jnp.clip(spiked(drawn, jax.random.fold_in(own_key, 3), *heavy), -most, most).astype(kind)


def setup_inputs(seed: int = 0) -> dict:
    arg_keys = jax.random.split(jax.random.key(seed), 9)
    tokens = noise_with(arg_keys[0], (TOKENS, D), 1.0, 6.0, ((0, 32),), (0, 1, 32, 2.75))
    up_gate = scatter_about(arg_keys[1], (TOKENS, FF), 1.5, 8.0, ((0, 4), (1, 8)))
    up_val = scatter_about(arg_keys[2], (TOKENS, FF), 1.0, 6.0, ((0, 4), (1, 8)))
    gate_weight = scatter_about(arg_keys[3], (D, FF), D ** -0.5, 0.125, ((0, 4), (1, 8)))
    val_weight = scatter_about(arg_keys[4], (D, FF), D ** -0.5, 0.125, ((0, 4), (1, 8)))
    gate_taps = scatter_about(arg_keys[5], (TAPS, FF), 0.6, 3.0, ((1, 8),))
    val_taps = scatter_about(arg_keys[6], (TAPS, FF), 0.6, 3.0, ((1, 8),))
    hidden_grad = noise_with(arg_keys[7], (TOKENS, FF), 1.0, 6.0, ((0, 4), (1, 8)), (0, 1, 8, 2.0))
    return {"tokens": tokens, "up_gate": up_gate, "up_val": up_val, "gate_weight": gate_weight, "val_weight": val_weight, "gate_taps": gate_taps, "val_taps": val_taps, "hidden_grad": hidden_grad}


def shifted_sum(padded, kernel, length, backward):
    tap_count = kernel.shape[0]
    result = jnp.zeros((padded.shape[0], length, padded.shape[2]), jnp.float32)
    for tap_index in range(tap_count):
        tap_shift = tap_count - 1 - tap_index if backward else tap_index
        result = result + kernel[tap_index][None, None, :] * padded[:, tap_shift:tap_shift + length]
    return result


def local_grads(up_gate, up_val, hidden_grad, gate_taps, val_taps):
    length = up_gate.shape[1]
    tap_count = gate_taps.shape[0]
    gate_kernel = gate_taps.astype(jnp.float32)
    val_kernel = val_taps.astype(jnp.float32)
    pad_front = ((0, 0), (tap_count - 1, 0), (0, 0))
    pad_back = ((0, 0), (0, tap_count - 1), (0, 0))
    padded_gate = jnp.pad(up_gate.astype(jnp.float32), pad_front)
    padded_val = jnp.pad(up_val.astype(jnp.float32), pad_front)
    conv_gate = shifted_sum(padded_gate, gate_kernel, length, False)
    conv_val = shifted_sum(padded_val, val_kernel, length, False)
    sigmoid_gate = jax.nn.sigmoid(conv_gate)
    grad_hidden = hidden_grad.astype(jnp.float32)
    val_back = grad_hidden * conv_gate * sigmoid_gate
    gate_back = grad_hidden * conv_val * sigmoid_gate * (1.0 + conv_gate * (1.0 - sigmoid_gate))
    up_gate_back = shifted_sum(jnp.pad(gate_back, pad_back), gate_kernel, length, True).astype(jnp.bfloat16)
    up_val_back = shifted_sum(jnp.pad(val_back, pad_back), val_kernel, length, True).astype(jnp.bfloat16)
    tap_gate = jnp.stack([jnp.sum(padded_gate[:, tap_index:tap_index + length] * gate_back, axis=(0, 1))
                          for tap_index in range(tap_count)])
    tap_val = jnp.stack([jnp.sum(padded_val[:, tap_index:tap_index + length] * val_back, axis=(0, 1))
                         for tap_index in range(tap_count)])
    return up_gate_back, up_val_back, tap_gate, tap_val


def reference(tokens, up_gate, up_val, gate_weight, val_weight, gate_taps, val_taps, hidden_grad):
    width_in = tokens.shape[1]
    hidden_units = up_gate.shape[1]
    block_width = hidden_units // N_TP
    seq_count = tokens.shape[0] // SEQ
    gate_float = gate_weight.astype(jnp.float32).reshape(width_in, N_TP, block_width)
    val_float = val_weight.astype(jnp.float32).reshape(width_in, N_TP, block_width)

    def slice_rows(values, row_start):
        return lax.dynamic_slice_in_dim(values, row_start, SEQ, 0)

    def one_sequence(totals, seq_index):
        row_start = (seq_index * SEQ).astype(jnp.int32)
        local_back = local_grads(slice_rows(up_gate, row_start)[None], slice_rows(up_val, row_start)[None],
                                 slice_rows(hidden_grad, row_start)[None], gate_taps, val_taps)
        gate_back = local_back[0][0]
        val_back = local_back[1][0]
        rows_in = slice_rows(tokens, row_start)
        gate_total = totals[0] + jnp.dot(rows_in.T, gate_back, preferred_element_type=jnp.float32)
        val_total = totals[1] + jnp.dot(rows_in.T, val_back, preferred_element_type=jnp.float32)
        tap_gate_total = totals[2] + local_back[2]
        tap_val_total = totals[3] + local_back[3]
        partials = jnp.einsum('sjf,djf->jsd', gate_back.astype(jnp.float32).reshape(SEQ, N_TP, block_width), gate_float)
        partials = partials + jnp.einsum('sjf,djf->jsd', val_back.astype(jnp.float32).reshape(SEQ, N_TP, block_width), val_float)
        rounded = lax.optimization_barrier(partials.astype(jnp.bfloat16))
        input_rows = jnp.sum(rounded.astype(jnp.float32), axis=0).astype(jnp.bfloat16)
        return (gate_total, val_total, tap_gate_total, tap_val_total), input_rows

    tap_count = gate_taps.shape[0]
    init = (jnp.zeros((width_in, hidden_units), jnp.float32), jnp.zeros((width_in, hidden_units), jnp.float32),
            jnp.zeros((tap_count, hidden_units), jnp.float32), jnp.zeros((tap_count, hidden_units), jnp.float32))
    totals, input_rows = lax.scan(one_sequence, init, jnp.arange(seq_count, dtype=jnp.int32))
    gate_grad, val_grad, tap_gate, tap_val = totals
    input_grad = input_rows.reshape(tokens.shape)
    gate_norms = jnp.sum(gate_grad * gate_grad, axis=1)
    val_norms = jnp.sum(val_grad * val_grad, axis=1)
    tap_norms = jnp.stack([jnp.sum(tap_gate * tap_gate, axis=1), jnp.sum(tap_val * tap_val, axis=1)])
    return (input_grad, gate_grad, val_grad, tap_gate, tap_val, gate_norms, val_norms, tap_norms)
```

```python
import jax
import jax.numpy as jnp
from jax import lax
from jax.sharding import PartitionSpec as P

SEQ = 1024


def masks_of(count):
    return [1 << bit for bit in range(count.bit_length() - 1)]


def mask_orders(count):
    masks = masks_of(count)
    middle = len(masks) // 2
    low, high = masks[:middle], masks[middle:]
    return low + high, high + low


def exchange(values, axis_name, count, mask):
    return lax.ppermute(values, axis_name, [(index, index ^ mask) for index in range(count)])


def butterfly_sum(values, axis_name, count):
    if count & (count - 1):
        return lax.psum(values, axis_name)
    for mask in masks_of(count):
        values = values + exchange(values, axis_name, count, mask)
    return values


def gather_blocks(block, axis_name, count, masks):
    held = {0: block}
    for mask in masks:
        arrived = {
            offset ^ mask: exchange(values, axis_name, count, mask)
            for offset, values in held.items()
        }
        held.update(arrived)
    return held


def shifted_sum(padded, kernel, length, backward):
    tap_count = kernel.shape[0]
    result = jnp.zeros((padded.shape[0], length, padded.shape[2]), jnp.float32)
    for tap_index in range(tap_count):
        tap_shift = tap_count - 1 - tap_index if backward else tap_index
        result = (
            result + kernel[tap_index][None, None, :] * padded[:, tap_shift : tap_shift + length]
        )
    return result


def local_grads(up_gate, up_val, hidden_grad, gate_taps, val_taps):
    length = up_gate.shape[1]
    tap_count = gate_taps.shape[0]
    gate_kernel = gate_taps.astype(jnp.float32)
    val_kernel = val_taps.astype(jnp.float32)
    pad_front = ((0, 0), (tap_count - 1, 0), (0, 0))
    pad_back = ((0, 0), (0, tap_count - 1), (0, 0))
    padded_gate = jnp.pad(up_gate.astype(jnp.float32), pad_front)
    padded_val = jnp.pad(up_val.astype(jnp.float32), pad_front)
    conv_gate = shifted_sum(padded_gate, gate_kernel, length, False)
    conv_val = shifted_sum(padded_val, val_kernel, length, False)
    sigmoid_gate = jax.nn.sigmoid(conv_gate)
    grad_hidden = hidden_grad.astype(jnp.float32)
    val_back = grad_hidden * conv_gate * sigmoid_gate
    gate_back = grad_hidden * conv_val * sigmoid_gate * (1.0 + conv_gate * (1.0 - sigmoid_gate))
    up_gate_back = shifted_sum(jnp.pad(gate_back, pad_back), gate_kernel, length, True).astype(
        jnp.bfloat16
    )
    up_val_back = shifted_sum(jnp.pad(val_back, pad_back), val_kernel, length, True).astype(
        jnp.bfloat16
    )
    taps_grad = [
        jnp.sum(padded[:, tap_index : tap_index + length] * back, axis=(0, 1))
        for padded, back in ((padded_gate, gate_back), (padded_val, val_back))
        for tap_index in range(tap_count)
    ]
    return up_gate_back, up_val_back, jnp.stack(taps_grad)


WEIGHT_CONTRACT = (((0,), (0,)), ((), ()))
INPUT_CONTRACT = (((1,), (1,)), ((), ()))


def dot(left, right, contract):
    return lax.dot_general(left, right, contract, preferred_element_type=jnp.float32)


def reduced_grad(token_rows, back, count, masks, rows):
    me = lax.axis_index("fs")
    order = sorted(range(count), key=lambda offset: -bin(offset).count("1"))
    partial = {}
    for offset in order:
        columns = lax.dynamic_slice_in_dim(token_rows, (me ^ offset) * rows, rows, 1)
        partial[offset] = dot(columns, back, WEIGHT_CONTRACT)
    for mask in masks:
        leaving = [offset for offset in partial if offset & mask]
        for offset in leaving:
            sent = partial.pop(offset).astype(jnp.bfloat16)
            arrived = exchange(sent, "fs", count, mask)
            partial[offset ^ mask] = partial[offset ^ mask] + arrived.astype(jnp.float32)
    return partial[0]


def make_local(fs_count, tp_count):
    gate_masks, val_masks = mask_orders(fs_count)

    def local(tokens, up_gate, up_val, gate_weight, val_weight, gate_taps, val_taps, hidden_grad):
        seq_count = up_gate.shape[0] // SEQ
        tap_count = gate_taps.shape[0]
        rows = gate_weight.shape[0]

        def as_blocks(values):
            return values.reshape(seq_count, SEQ, values.shape[1])

        token_rows = lax.all_gather(tokens, "tp", axis=0, tiled=True)
        gate_blocks = gather_blocks(gate_weight, "fs", fs_count, gate_masks)
        val_blocks = gather_blocks(val_weight, "fs", fs_count, val_masks)
        gate_back, val_back, taps_grad = local_grads(
            as_blocks(up_gate), as_blocks(up_val), as_blocks(hidden_grad), gate_taps, val_taps
        )
        gate_back = gate_back.reshape(up_gate.shape)
        val_back = val_back.reshape(up_val.shape)
        taps_grad = butterfly_sum(taps_grad, "fs", fs_count)
        tap_gate, tap_val = taps_grad[:tap_count], taps_grad[tap_count:]
        tap_norms = butterfly_sum(jnp.sum(taps_grad * taps_grad, axis=1), "tp", tp_count)

        gate_grad = reduced_grad(token_rows, gate_back, fs_count, gate_masks, rows)
        val_grad = reduced_grad(token_rows, val_back, fs_count, val_masks, rows)

        partials = [
            (
                dot(gate_back, gate_blocks[offset], INPUT_CONTRACT)
                + dot(val_back, val_blocks[offset], INPUT_CONTRACT)
            ).astype(jnp.bfloat16)
            for offset in range(fs_count)
        ]
        mixed = lax.psum_scatter(
            jnp.concatenate(partials, axis=1), "tp", scatter_dimension=0, tiled=True
        )
        me = lax.axis_index("fs")
        input_grad = jnp.concatenate(
            [
                lax.dynamic_slice_in_dim(mixed, (me ^ block) * rows, rows, 1)
                for block in range(fs_count)
            ],
            axis=1,
        )
        norms = jnp.stack(
            [jnp.sum(gate_grad * gate_grad, axis=1), jnp.sum(val_grad * val_grad, axis=1)]
        )
        norms = butterfly_sum(norms, "tp", tp_count)
        return (
            input_grad,
            gate_grad,
            val_grad,
            tap_gate,
            tap_val,
            norms[0],
            norms[1],
            tap_norms.reshape(2, tap_count),
        )

    return local


def solution(mesh):
    in_specs = (
        P(("fs", "tp"), None),
        P("fs", "tp"),
        P("fs", "tp"),
        P("fs", "tp"),
        P("fs", "tp"),
        P(None, "tp"),
        P(None, "tp"),
        P("fs", "tp"),
    )
    out_specs = (
        P(("fs", "tp"), None),
        P("fs", "tp"),
        P("fs", "tp"),
        P(None, "tp"),
        P(None, "tp"),
        P("fs"),
        P("fs"),
        P(),
    )
    local = make_local(mesh.shape["fs"], mesh.shape["tp"])
    return jax.shard_map(
        local, mesh=mesh, in_specs=in_specs, out_specs=out_specs, check_vma=False
    )
```

```python
import jax
import jax.numpy as jnp
from jax import lax
from jax.sharding import PartitionSpec as P


SEQ = 1024


def masks_of(count):
    return [1 << bit for bit in range(count.bit_length() - 1)]


def mask_orders(count):
    masks = masks_of(count)
    middle = len(masks) // 2
    low, high = masks[:middle], masks[middle:]
    return low + high, high + low


def exchange(values, axis_name, count, mask):
    return lax.ppermute(values, axis_name, [(index, index ^ mask) for index in range(count)])


def butterfly_sum(values, axis_name, count):
    if count & (count - 1):
        return lax.psum(values, axis_name)
    for mask in masks_of(count):
        arrived = exchange(values, axis_name, count, mask)
        values = values + arrived
    return values


def gather_blocks(block, axis_name, count, masks):
    held = {0: block}
    for mask in masks:
        arrived = {
            offset ^ mask: exchange(values, axis_name, count, mask)
            for offset, values in held.items()
        }
        held.update(arrived)
    return held


def shifted_sum(padded, kernel, length, backward):
    tap_count = kernel.shape[0]
    result = jnp.zeros((padded.shape[0], length, padded.shape[2]), jnp.float32)
    for tap_index in range(tap_count):
        tap_shift = tap_count - 1 - tap_index if backward else tap_index
        result = (
            result + kernel[tap_index][None, None, :] * padded[:, tap_shift : tap_shift + length]
        )
    return result


def local_grads(up_gate, up_val, hidden_grad, gate_taps, val_taps):
    length = up_gate.shape[1]
    tap_count = gate_taps.shape[0]
    gate_kernel = gate_taps.astype(jnp.float32)
    val_kernel = val_taps.astype(jnp.float32)
    pad_front = ((0, 0), (tap_count - 1, 0), (0, 0))
    pad_back = ((0, 0), (0, tap_count - 1), (0, 0))
    padded_gate = jnp.pad(up_gate.astype(jnp.float32), pad_front)
    padded_val = jnp.pad(up_val.astype(jnp.float32), pad_front)
    conv_gate = shifted_sum(padded_gate, gate_kernel, length, False)
    conv_val = shifted_sum(padded_val, val_kernel, length, False)
    sigmoid_gate = jax.nn.sigmoid(conv_gate)
    grad_hidden = hidden_grad.astype(jnp.float32)
    val_back = grad_hidden * conv_gate * sigmoid_gate
    gate_back = grad_hidden * conv_val * sigmoid_gate * (1.0 + conv_gate * (1.0 - sigmoid_gate))
    up_gate_back = shifted_sum(jnp.pad(gate_back, pad_back), gate_kernel, length, True).astype(
        jnp.bfloat16
    )
    up_val_back = shifted_sum(jnp.pad(val_back, pad_back), val_kernel, length, True).astype(
        jnp.bfloat16
    )
    taps_grad = [
        jnp.sum(padded[:, tap_index : tap_index + length] * back, axis=(0, 1))
        for padded, back in ((padded_gate, gate_back), (padded_val, val_back))
        for tap_index in range(tap_count)
    ]
    return up_gate_back, up_val_back, jnp.stack(taps_grad)


WEIGHT_CONTRACT = (((0,), (0,)), ((), ()))
INPUT_CONTRACT = (((1,), (1,)), ((), ()))


def dot(left, right, contract):
    return lax.dot_general(left, right, contract, preferred_element_type=jnp.float32)


def tie(values, after):
    return lax.optimization_barrier((values, after))[0]


def scatter_blocks(partial, sent, axis_name, count, masks):
    for mask in masks:
        leaving = [offset for offset in partial if offset & mask]
        for offset in leaving:
            values = partial.pop(offset)
            values = sent.get(offset, values.astype(jnp.bfloat16))
            arrived = exchange(values, axis_name, count, mask)
            target = offset ^ mask
            partial[target] = partial[target] + arrived.astype(jnp.float32)
            sent.pop(target, None)
    return partial[0]


def make_local(fs_count, tp_count):
    gate_masks, val_masks = mask_orders(fs_count)
    farthest_first = sorted(range(fs_count), key=lambda offset: -bin(offset).count("1"))

    def local(tokens, up_gate, up_val, gate_weight, val_weight, gate_taps, val_taps, hidden_grad):
        seq_count = up_gate.shape[0] // SEQ
        tap_count = gate_taps.shape[0]
        rows = gate_weight.shape[0]
        own_tokens = tokens.shape[0]
        me = lax.axis_index("fs")

        def as_blocks(values):
            return values.reshape(seq_count, SEQ, values.shape[1])

        token_rows = lax.all_gather(tokens, "tp", axis=0, tiled=True)
        gate_blocks = gather_blocks(gate_weight, "fs", fs_count, gate_masks)
        val_blocks = gather_blocks(val_weight, "fs", fs_count, val_masks)
        gate_back, val_back, taps_grad = local_grads(
            as_blocks(up_gate), as_blocks(up_val), as_blocks(hidden_grad), gate_taps, val_taps
        )
        gate_back = gate_back.reshape(up_gate.shape)
        val_back = val_back.reshape(up_val.shape)
        taps_grad = butterfly_sum(taps_grad, "fs", fs_count)
        tap_gate, tap_val = taps_grad[:tap_count], taps_grad[tap_count:]

        gate_partial, val_partial, gate_sent, val_sent = {}, {}, {}, {}
        for offset in farthest_first:
            columns = lax.dynamic_slice_in_dim(token_rows, (me ^ offset) * rows, rows, 1)
            gate_partial[offset] = dot(columns, gate_back, WEIGHT_CONTRACT)
            val_partial[offset] = dot(columns, val_back, WEIGHT_CONTRACT)
        far = farthest_first[0]
        if far:
            gate_sent[far] = gate_partial[far].astype(jnp.bfloat16)
            val_sent[far] = val_partial[far].astype(jnp.bfloat16)
            gate_blocks[far], val_blocks[far] = tie(
                (gate_blocks[far], val_blocks[far]), (gate_sent[far], val_sent[far])
            )

        shares = []
        for offset in range(fs_count):
            total = dot(gate_back, gate_blocks[offset], INPUT_CONTRACT)
            total = total + dot(val_back, val_blocks[offset], INPUT_CONTRACT)
            shares.append(total.astype(jnp.bfloat16).reshape(tp_count, own_tokens, rows))
        mixed = lax.psum_scatter(
            jnp.stack(shares, axis=1).reshape(-1, rows), "tp", scatter_dimension=0, tiled=True
        ).reshape(fs_count, own_tokens, rows)
        gate_grad = scatter_blocks(gate_partial, gate_sent, "fs", fs_count, gate_masks)
        val_grad = scatter_blocks(val_partial, val_sent, "fs", fs_count, val_masks)
        input_grad = jnp.concatenate(
            [
                lax.dynamic_index_in_dim(mixed, me ^ block, 0, keepdims=False)
                for block in range(fs_count)
            ],
            axis=1,
        )
        norms = jnp.concatenate(
            [
                jnp.sum(gate_grad * gate_grad, axis=1),
                jnp.sum(val_grad * val_grad, axis=1),
                jnp.sum(taps_grad * taps_grad, axis=1),
            ]
        )
        norms = butterfly_sum(norms, "tp", tp_count)
        return (
            input_grad,
            gate_grad,
            val_grad,
            tap_gate,
            tap_val,
            norms[:rows],
            norms[rows : 2 * rows],
            norms[2 * rows :].reshape(2, tap_count),
        )

    return local


def solution(mesh):
    in_specs = (
        P(("fs", "tp"), None),
        P("fs", "tp"),
        P("fs", "tp"),
        P("fs", "tp"),
        P("fs", "tp"),
        P(None, "tp"),
        P(None, "tp"),
        P("fs", "tp"),
    )
    out_specs = (
        P(("fs", "tp"), None),
        P("fs", "tp"),
        P("fs", "tp"),
        P(None, "tp"),
        P(None, "tp"),
        P("fs"),
        P("fs"),
        P(),
    )
    fs_count = mesh.shape["fs"]
    local = make_local(fs_count, mesh.shape["tp"])
    return jax.shard_map(
        local, mesh=mesh, in_specs=in_specs, out_specs=out_specs, check_vma=False
    )
```
